32 devices in a mesh: grp: 2 (over y), fs: 4 (over z), tp: 4 (over x, core).
Axes of the slice: x: 2, y: 2, z: 4, core: 2. Of those that a mesh axis runs over, the one named last changes fastest.
Arguments:
- tokens: bfloat16 [32, 128, 2048], P(('grp', 'fs'), None, 'tp'), parts along dimension 0, may hold values from -100 to 100
- mix_gain: float32 [2048], replicated, may hold values from 0.1 to 1.9
- gate_outer: bfloat16 [2048, 1024], P('fs', 'tp'), may hold values from -0.125 to 0.125
- gate_inner: bfloat16 [2048, 1024], P('fs', 'tp'), may hold values from -0.125 to 0.125
- value_weight: bfloat16 [2048, 1024], P('fs', 'tp'), may hold values from -0.125 to 0.125
- conv_taps: float32 [3, 1024], replicated, may hold values from -3 to 3
- mix_out: bfloat16 [1024, 2048], P('tp', 'fs'), may hold values from -0.25 to 0.25
- ffn_gain: float32 [2048], replicated, may hold values from 0.1 to 1.9
- ffn_gate: bfloat16 [2048, 5632], P('fs', 'tp'), may hold values from -0.125 to 0.125
- ffn_up: bfloat16 [2048, 5632], P('fs', 'tp'), may hold values from -0.125 to 0.125
- ffn_down: bfloat16 [5632, 2048], P('tp', 'fs'), may hold values from -0.109375 to 0.109375
- out_gain: float32 [2048], replicated, may hold values from 0.1 to 1.9
Outputs:
- layer_out: bfloat16 [32, 128, 2048], P(('grp', 'fs'), None, 'tp'), parts along dimension 0
The draws below stay inside these ranges and needn't reach their ends.
There are 2 independent parts, one for each index of `grp`. The reference program is written for one: setup_inputs(seed, part) draws one part's arguments, and reference() takes and returns one part's arrays. A program takes and returns all parts, laid end to end along the dimension named above; an argument that names none is the same for every part. Nothing has to cross between parts.
All inputs are finite; a program needn't handle non-finite values.
Results may differ from the reference program's by a relative error of at most 0.015.
Values may be sent and summed in bfloat16 or wider, within the bound.
No kernel may reach another device: no remote copies, remote signals or barrier semaphores. Data moves between devices by JAX's collectives and lax.ppermute only.
A program may use at most 64 MiB of HBM per device.

```python
import math
import jax
import jax.numpy as jnp
from jax import lax

D = 2048
CA = 1024
FF = 5632
TAPS = 3
LEN = 128
SEQS = 16
N_TP = 4


def draw_tokens(key, part):
    first_key, second_key = jax.random.split(jax.random.fold_in(key, 11), 2)
    ramp = jnp.exp(jnp.linspace(math.log(0.4), math.log(4.0), D)).astype(jnp.float32)
    rough = jax.random.uniform(second_key, (D,), jnp.float32, 0.6, 1.4)
    values = jax.random.normal(first_key, (SEQS, LEN, D), jnp.float32) * ramp * rough
    return jnp.clip(values, -100.0, 100.0).astype(jnp.bfloat16)


def with_spikes(drawn, own_key, source, target, parts, factor):
    owner, partner = [(jnp.arange(drawn.shape[dim]) // (drawn.shape[dim] // parts)).reshape([-1 if axis == dim else 1 for axis in range(drawn.ndim)]) for dim in (source, target)]
    chosen = jax.random.permutation(own_key, parts)[partner]
    strong = (owner == chosen) | (owner == (partner + parts // 2) % parts)
    return jnp.where(strong, factor * drawn, drawn)


def block_levels(stream_key, dims, cuts, low, largest):
    factor_of, own = 1.0, jax.random.fold_in(stream_key, 6)
    for axis_at, shards_of in cuts:
        draws = jnp.exp(jax.random.uniform(jax.random.fold_in(own, axis_at), (shards_of,), jnp.float32, low / len(cuts), largest / len(cuts)))
        factor_of = factor_of * jnp.repeat(draws, dims[axis_at] // shards_of).reshape([-1 if axis == axis_at else 1 for axis in range(len(dims))])
    return factor_of


def centred(own_key, dims, spread, limit, cuts=(), held_as=jnp.bfloat16):
    values = spread * jax.random.normal(own_key, dims, jnp.float32)
    if cuts:
        values = values * block_levels(own_key, dims, cuts, -0.22, 0.18)
    return jnp.clip(values, -limit, limit).astype(held_as)


def gaussian_with(key, extent, scale, limit, pieces, heavy, held_as=jnp.bfloat16):
    result = scale * jax.random.normal(key, extent, jnp.float32)
    if pieces:
        result = result * block_levels(key, extent, pieces, -0.22, 0.18)
    return jnp.clip(with_spikes(result, jax.random.fold_in(key, 3), *heavy), -limit, limit).astype(held_as)


def setup_inputs(seed: int = 0, part: int = 0) -> dict:
    streams_of = jax.random.split(jax.random.key(seed), 13)
    part_splits = jax.random.split(jax.random.fold_in(streams_of[12], part), 13)
    return {
        "tokens": draw_tokens(jax.random.fold_in(jax.random.fold_in(streams_of[12], part), 71), part),
        "mix_gain": jnp.clip(1.0 + 0.18 * jax.random.normal(streams_of[1], (D,), jnp.float32), 0.1, 1.9),
        "gate_outer": centred(streams_of[2], (D, CA), D ** -0.5, 0.125, ((0, 4), (1, 4))),
        "gate_inner": centred(streams_of[3], (D, CA), D ** -0.5, 0.125, ((0, 4), (1, 4))),
        "value_weight": centred(streams_of[4], (D, CA), D ** -0.5, 0.125, ((0, 4), (1, 4))),
        "conv_taps": centred(streams_of[5], (TAPS, CA), 0.6, 3.0, (), jnp.float32),
        "mix_out": gaussian_with(streams_of[6], (CA, D), CA ** -0.5, 0.25, ((0, 4), (1, 4)), (0, 1, 4, 2.0)),
        "ffn_gain": jnp.clip(1.0 + 0.18 * jax.random.normal(streams_of[7], (D,), jnp.float32), 0.1, 1.9),
        "ffn_gate": centred(streams_of[8], (D, FF), D ** -0.5, 0.125, ((0, 4), (1, 4))),
        "ffn_up": centred(streams_of[9], (D, FF), D ** -0.5, 0.125, ((0, 4), (1, 4))),
        "ffn_down": gaussian_with(streams_of[10], (FF, D), FF ** -0.5, 0.109375, ((0, 4), (1, 4)), (0, 1, 4, 2.0)),
        "out_gain": jnp.clip(1.0 + 0.18 * jax.random.normal(streams_of[11], (D,), jnp.float32), 0.1, 1.9),
    }


def rms_norm(values, gain):
    floats = values.astype(jnp.float32)
    scaled = floats * lax.rsqrt(lax.optimization_barrier(jnp.mean(floats * floats, axis=-1, keepdims=True)) + 1e-06)
    return scaled * gain.astype(jnp.float32)

def blocked_sum(left, weight, blocks):
    width = left.shape[1] // blocks
    summed = jnp.zeros((left.shape[0], weight.shape[1]), jnp.float32)
    for number in range(blocks):
        partial_value = jnp.dot(left[:, number * width:(number + 1) * width], weight[number * width:(number + 1) * width], preferred_element_type=jnp.float32).astype(jnp.bfloat16)
        summed = summed + lax.optimization_barrier(partial_value).astype(jnp.float32)
    return summed

def reference(tokens, mix_gain, gate_outer, gate_inner, value_weight, conv_taps, mix_out, ffn_gain, ffn_gate, ffn_up, ffn_down, out_gain):
    rows = SEQS * LEN
    flat = tokens.reshape(rows, D)
    normed = rms_norm(flat, mix_gain).astype(jnp.bfloat16)
    outer = jnp.dot(normed, gate_outer, preferred_element_type=jnp.float32).astype(jnp.bfloat16)
    inner = jnp.dot(normed, gate_inner, preferred_element_type=jnp.float32).astype(jnp.bfloat16)
    values = jnp.dot(normed, value_weight, preferred_element_type=jnp.float32).astype(jnp.bfloat16)
    product = (inner.astype(jnp.float32) * values.astype(jnp.float32)).reshape(SEQS, LEN, CA)
    padded = jnp.pad(product, ((0, 0), (TAPS - 1, 0), (0, 0)))
    conv = jnp.zeros((SEQS, LEN, CA), jnp.float32)
    for offset in range(TAPS):
        conv = conv + conv_taps[offset].astype(jnp.float32) * padded[:, offset:offset + LEN]
    gated = (outer.astype(jnp.float32) * conv.reshape(rows, CA)).astype(jnp.bfloat16)
    first = (flat.astype(jnp.float32) + blocked_sum(gated, mix_out, N_TP)).astype(jnp.bfloat16)
    normed_ffn = rms_norm(first, ffn_gain).astype(jnp.bfloat16)
    gate = jnp.dot(normed_ffn, ffn_gate, preferred_element_type=jnp.float32)
    upward = jnp.dot(normed_ffn, ffn_up, preferred_element_type=jnp.float32)
    hidden = (jax.nn.silu(gate) * upward).astype(jnp.bfloat16)
    second = first.astype(jnp.float32) + blocked_sum(hidden, ffn_down, N_TP)
    return rms_norm(second, out_gain).astype(jnp.bfloat16).reshape(SEQS, LEN, D)
```

```python
import functools

import jax
import jax.numpy as jnp
from jax import lax
from jax.experimental import pallas as pl
from jax.experimental.pallas import tpu as pltpu
from jax.sharding import PartitionSpec as P


BF16 = jnp.bfloat16
F32 = jnp.float32
VMEM_LIMIT = 56 * 1024 * 1024


def rms_norm(values, gain):
    floats = values.astype(F32)
    scaled = floats * lax.rsqrt(jnp.mean(floats * floats, axis=-1, keepdims=True) + 1e-06)
    return (scaled * gain).astype(BF16)


def plain_local(
    tokens, mix_gain, gate_outer, gate_inner, value_weight, conv_taps, mix_out,
    ffn_gain, ffn_gate, ffn_up, ffn_down, out_gain,
):
    seq_count, length, columns = tokens.shape
    row_count = seq_count * length
    width = columns * lax.axis_size("tp")
    whole = lax.all_gather(tokens, "tp", axis=2, tiled=True).reshape(row_count, width)
    normed = rms_norm(whole, mix_gain)
    channels = gate_outer.shape[1]

    def project(left, weight):
        full = lax.all_gather(weight, "fs", axis=0, tiled=True)
        return jnp.dot(left, full, preferred_element_type=F32)

    outer = project(normed, gate_outer).astype(BF16)
    inner = project(normed, gate_inner).astype(BF16)
    values = project(normed, value_weight).astype(BF16)
    product = (inner.astype(F32) * values.astype(F32)).reshape(seq_count, length, channels)
    own_taps = lax.dynamic_slice_in_dim(conv_taps, lax.axis_index("tp") * channels, channels, 1)
    tap_count = conv_taps.shape[0]
    padded = jnp.pad(product, ((0, 0), (tap_count - 1, 0), (0, 0)))
    conv = jnp.zeros((seq_count, length, channels), F32)
    for offset in range(tap_count):
        conv = conv + own_taps[offset] * padded[:, offset : offset + length]
    gated = (outer.astype(F32) * conv.reshape(row_count, channels)).astype(BF16)
    mix_terms = jnp.dot(
        gated, lax.all_gather(mix_out, "fs", axis=1, tiled=True), preferred_element_type=F32
    )
    mix_full = lax.psum(mix_terms.astype(BF16), "tp").astype(F32)
    first_full = (whole.astype(F32) + mix_full).astype(BF16)
    first = lax.dynamic_slice_in_dim(first_full, lax.axis_index("tp") * columns, columns, 1)
    normed_ffn = rms_norm(first_full, ffn_gain)
    gate = project(normed_ffn, ffn_gate)
    upward = project(normed_ffn, ffn_up)
    hidden = (jax.nn.silu(gate) * upward).astype(BF16)
    down_terms = jnp.dot(
        hidden, lax.all_gather(ffn_down, "fs", axis=1, tiled=True), preferred_element_type=F32
    )
    down_summed = lax.psum_scatter(
        down_terms.astype(BF16), "tp", scatter_dimension=1, tiled=True
    ).astype(F32)
    second = first.astype(F32) + down_summed
    squares = lax.psum(jnp.sum(second * second, axis=1), "tp")
    factor = lax.rsqrt(squares / width + 1e-06)
    own_gain = lax.dynamic_slice_in_dim(out_gain, lax.axis_index("tp") * columns, columns, 0)
    result = second * factor[:, None] * own_gain
    return result.astype(BF16).reshape(seq_count, length, columns)


def dot(left, right):
    return jnp.dot(left, right, preferred_element_type=F32)


def norm_kernel(info, gain, b0, b1, b2, b3, out, *, width):
    q = info[2]
    blocks = [b[h].astype(F32) for b in (b0, b1, b2, b3) for h in range(2)]
    squares = sum(jnp.sum(b * b, axis=-1, keepdims=True) for b in blocks)
    factor = lax.rsqrt(squares / width + 1e-06)
    for r in range(4):
        for h in range(2):
            own = gain[(q ^ r) * 2 + h]
            out[2 * r + h] = (blocks[2 * r + h] * factor * own).astype(BF16)


def norm_call(info, gain, blocks):
    _, rows, half = blocks[0].shape
    tile = min(rows, 128)
    width = 8 * half
    spec = pl.BlockSpec((2, tile, half), lambda i, s: (0, i, 0))
    return pl.pallas_call(
        functools.partial(norm_kernel, width=width),
        grid_spec=pltpu.PrefetchScalarGridSpec(
            num_scalar_prefetch=1,
            grid=(rows // tile,),
            in_specs=[pl.BlockSpec((8, 1, half), lambda i, s: (0, 0, 0))] + [spec] * 4,
            out_specs=pl.BlockSpec((8, tile, half), lambda i, s: (0, i, 0)),
        ),
        out_shape=jax.ShapeDtypeStruct((8, rows, half), BF16),
        cost_estimate=pl.CostEstimate(
            flops=4000000 * rows // 512, bytes_accessed=4 * rows * width, transcendentals=rows
        ),
        name="norm",
    )(info, gain.reshape(8, 1, half), *blocks)


def place(info, step, direction, count):
    z, q = info[0], info[2]
    shard = lax.rem(z + (count - step if direction > 0 else step), count)
    return shard ^ q


def contract(x, info, own, own_row, pieces, direction, count, row, columns):
    g = info[1]
    half = x.shape[2]
    total = None
    spot = place(info, 0, direction, count)
    for h in range(2):
        term = dot(x[2 * spot + h], own[own_row + h * half : own_row + (h + 1) * half, columns])
        total = term if total is None else total + term
    for step, swapped, piece in pieces:
        spot = place(info, step, direction, count)
        part = 1 - g if swapped else g
        total = total + dot(x[2 * spot + part], piece[row : row + half, :])
    return total


def mixer_kernel(*refs, count, length):
    info, taps, x, outer_own, inner_own, value_own, mix_own = refs[:7]
    steps = count - 1
    ahead, ahead_y = refs[7 : 7 + steps], refs[7 + steps : 7 + 2 * steps]
    back, back_y = refs[7 + 2 * steps : 7 + 3 * steps], refs[7 + 3 * steps : 7 + 4 * steps]
    out = refs[-1]
    half = x.shape[2]
    everything = slice(None)
    g = info[1]
    cw = [(k + 1, s, p) for s, group in ((False, ahead), (True, ahead_y)) for k, p in enumerate(group)]
    ccw = [(k + 1, s, p) for s, group in ((False, back), (True, back_y)) for k, p in enumerate(group)]
    inner = contract(x, info, inner_own, 0, cw, 1, count, 0, everything).astype(BF16)
    values = contract(x, info, value_own, 0, cw, 1, count, half, everything).astype(BF16)
    outer = contract(x, info, outer_own, 0, ccw, -1, count, 0, everything).astype(BF16)
    product = inner.astype(F32) * values.astype(F32)
    position = lax.broadcasted_iota(jnp.int32, product.shape, 0) % length
    tap_count = taps.shape[0]
    conv = jnp.zeros(product.shape, F32)
    for offset in range(tap_count):
        back_by = tap_count - 1 - offset
        if back_by:
            moved = pltpu.roll(product, back_by, axis=0)
            moved = jnp.where(position >= back_by, moved, 0.0)
        else:
            moved = product
        conv = conv + taps[offset][None, :] * moved
    gated = (outer.astype(F32) * conv).astype(BF16)

    def store(step, part, value):
        spot = place(info, step, -1, count)
        out[lax.rem(spot, 2), spot // 2, part] = value.astype(BF16)

    for h in range(2):
        store(0, h, dot(gated, mix_own[:, h * half : (h + 1) * half]))
    for step, swapped, piece in ccw:
        store(step, 1 - g if swapped else g, dot(gated, piece[half:, :]))


def full(shape):
    return pl.BlockSpec(shape, lambda *_: (0,) * len(shape))


def mixer_call(info, taps, x, owns, cw, cw_y, ccw, ccw_y, count, length):
    _, rows, half = x.shape
    tap_count = taps.shape[0]
    channels = owns[0].shape[1]
    operands = [x, *owns, *cw, *cw_y, *ccw, *ccw_y]
    return pl.pallas_call(
        functools.partial(mixer_kernel, count=count, length=length),
        grid_spec=pltpu.PrefetchScalarGridSpec(
            num_scalar_prefetch=1,
            grid=(1,),
            in_specs=[pl.BlockSpec((tap_count, channels), lambda i, s: (0, s[2]))]
            + [full(o.shape) for o in operands],
            out_specs=full((2, 2, 2, rows, half)),
        ),
        out_shape=jax.ShapeDtypeStruct((2, 2, 2, rows, half), BF16),
        cost_estimate=pl.CostEstimate(
            flops=8 * rows * 8 * half * channels, bytes_accessed=16000000, transcendentals=0
        ),
        compiler_params=pltpu.CompilerParams(vmem_limit_bytes=VMEM_LIMIT),
        name="mixer",
    )(info, taps, *operands)


def hidden_kernel(*refs, count, start, size):
    info, x, gate_own, up_own = refs[:4]
    steps = count - 1
    groups = [refs[4 + i * steps : 4 + (i + 1) * steps] for i in range(4)]
    out = refs[-1]
    columns = slice(start, start + size)
    cw = [(k + 1, i == 1, p) for i in (0, 1) for k, p in enumerate(groups[i])]
    ccw = [(k + 1, i == 3, p) for i in (2, 3) for k, p in enumerate(groups[i])]
    gate = contract(x, info, gate_own, 0, cw, 1, count, 0, columns)
    upward = contract(x, info, up_own, 0, ccw, -1, count, 0, columns)
    out[...] = (gate / (1.0 + jnp.exp(-gate)) * upward).astype(BF16)


def hidden_call(info, x, gate_own, up_own, cw, cw_y, ccw, ccw_y, count, start, size):
    _, rows, half = x.shape
    operands = [gate_own, up_own, *cw, *cw_y, *ccw, *ccw_y]
    tile = min(rows, 256)
    return pl.pallas_call(
        functools.partial(hidden_kernel, count=count, start=start, size=size),
        grid_spec=pltpu.PrefetchScalarGridSpec(
            num_scalar_prefetch=1,
            grid=(rows // tile,),
            in_specs=[pl.BlockSpec((8, tile, half), lambda i, s: (0, i, 0))]
            + [full(o.shape) for o in operands],
            out_specs=pl.BlockSpec((tile, size), lambda i, s: (i, 0)),
        ),
        out_shape=jax.ShapeDtypeStruct((rows, size), BF16),
        cost_estimate=pl.CostEstimate(
            flops=4 * rows * 8 * half * size,
            bytes_accessed=4 * 8 * half * size,
            transcendentals=rows * size,
        ),
        compiler_params=pltpu.CompilerParams(vmem_limit_bytes=VMEM_LIMIT),
        name="hidden",
    )(info, x, *operands)


def down_kernel(*refs, count, split):
    info, left, right, own = refs[:4]
    steps = count - 1
    groups = [refs[4 + i * steps : 4 + (i + 1) * steps] for i in range(4)]
    out = refs[-1]
    g = info[1]
    piece = out.shape[-1]

    def product(weight):
        return dot(left[...], weight[:split]) + dot(right[...], weight[split:])

    def store(spot, part, value):
        out[lax.rem(spot, 2), spot // 2, part] = value.astype(BF16)

    for h in range(2):
        value = product(own[:, 2 * h * piece : 2 * (h + 1) * piece])
        for i in range(2):
            store(place(info, 0, 1, count), 2 * h + i, value[:, i * piece : (i + 1) * piece])
    for k in range(steps):
        for direction, mine, other in ((1, groups[0][k], groups[1][k]), (-1, groups[2][k], groups[3][k])):
            value = product(jnp.concatenate([mine[...], other[...]], axis=1))
            spot = place(info, k + 1, direction, count)
            last = 0 if direction > 0 else 1
            store(spot, 2 * g + last, value[:, :piece])
            store(spot, 2 * (1 - g) + last, value[:, piece:])


def down_call(info, left, right, own, cw, cw_y, ccw, ccw_y, count):
    rows, split = left.shape
    piece = cw[0].shape[1]
    operands = [left, right, own, *cw, *cw_y, *ccw, *ccw_y]
    return pl.pallas_call(
        functools.partial(down_kernel, count=count, split=split),
        grid_spec=pltpu.PrefetchScalarGridSpec(
            num_scalar_prefetch=1,
            grid=(1,),
            in_specs=[full(o.shape) for o in operands],
            out_specs=full((2, 2, 4, rows, piece)),
        ),
        out_shape=jax.ShapeDtypeStruct((2, 2, 4, rows, piece), BF16),
        cost_estimate=pl.CostEstimate(
            flops=2 * rows * own.shape[0] * 16 * piece,
            bytes_accessed=2 * own.shape[0] * 16 * piece,
            transcendentals=0,
        ),
        compiler_params=pltpu.CompilerParams(vmem_limit_bytes=VMEM_LIMIT),
        name="down",
    )(info, *operands)


def ring_local(
    tokens, mix_gain, gate_outer, gate_inner, value_weight, conv_taps, mix_out,
    ffn_gain, ffn_gate, ffn_up, ffn_down, out_gain,
):
    count = lax.axis_size("fs")
    seq_count, length, columns = tokens.shape
    rows = seq_count * length
    half = columns // 2
    width = columns * lax.axis_size("tp")
    z, g, q = lax.axis_index("fs"), lax.axis_index("grp"), lax.axis_index("tp")
    info = jnp.stack([z, g, q]).astype(jnp.int32)

    ahead = [(i, (i + 1) % count) for i in range(count)]
    behind = [(d, s) for s, d in ahead]

    def ring(value, pairs):
        arrived, swapped = [], []
        for _ in range(1, count):
            value = lax.ppermute(value, "fs", pairs)
            arrived.append(value)
            swapped.append(lax.ppermute(value, "grp", [(0, 1), (1, 0)]))
        return arrived, swapped

    def mate(value):
        return lax.ppermute(value, "tp", [(i, i ^ 1) for i in range(4)])

    def across(value):
        return lax.ppermute(value, "tp", [(i, i ^ 2) for i in range(4)])

    def gather(own):
        other = across(own)
        return own, mate(own), other, mate(other)

    def rows_of(weight):
        return lax.dynamic_slice_in_dim(weight, g * half, half, 0)

    own_tokens = tokens.reshape(rows, 2, half).transpose(1, 0, 2)
    blocks = gather(own_tokens)

    mix_half = lax.dynamic_slice_in_dim(mix_out, g * half, half, 1)
    m_cw = ring(jnp.concatenate([rows_of(gate_inner), rows_of(value_weight)]), ahead)
    m_ccw = ring(jnp.concatenate([rows_of(gate_outer), mix_half]), behind)
    units = ffn_gate.shape[1]
    split = -(-units // 256) * 128
    gate_half, up_half = rows_of(ffn_gate), rows_of(ffn_up)
    g1 = ring(gate_half[:, :split], ahead)
    u1 = ring(up_half[:, :split], behind)
    g2 = ring(gate_half[:, split:], ahead)
    u2 = ring(up_half[:, split:], behind)
    down_half = lax.dynamic_slice_in_dim(ffn_down, g * half, half, 1)
    d_cw = ring(down_half[:, : half // 2], ahead)
    d_ccw = ring(down_half[:, half // 2 :], behind)

    def scatter(partial):
        met = partial[0].astype(F32) + mate(partial[1]).astype(F32)
        return met[0] + across(met[1].astype(BF16)).astype(F32)

    x = norm_call(info, mix_gain, blocks)
    partial = mixer_call(
        info, conv_taps, x, (gate_outer, gate_inner, value_weight, mix_out), *m_cw, *m_ccw, count, length
    )
    first = (own_tokens.astype(F32) + scatter(partial)).astype(BF16)
    x = norm_call(info, ffn_gain, gather(first))
    left = hidden_call(info, x, ffn_gate, ffn_up, *g1, *u1, count, 0, split)
    right = hidden_call(info, x, ffn_gate, ffn_up, *g2, *u2, count, split, units - split)
    partial = down_call(info, left, right, ffn_down, *d_cw, *d_ccw, count)
    summed = scatter(partial)
    second = first.transpose(1, 0, 2).reshape(rows, columns).astype(F32)
    second = second + summed.transpose(1, 0, 2).reshape(rows, columns)
    squares = lax.psum(jnp.sum(second * second, axis=1), "tp")
    factor = lax.rsqrt(squares / width + 1e-06)
    own_gain = lax.dynamic_slice_in_dim(out_gain, q * columns, columns, 0)
    result = second * factor[:, None] * own_gain
    return result.astype(BF16).reshape(seq_count, length, columns)


def fits_ring(mesh):
    shape = mesh.shape
    return shape["grp"] == 2 and shape["tp"] == 4 and shape["fs"] == 4


def solution(mesh):
    in_specs = (
        P(("grp", "fs"), None, "tp"),
        P(),
        P("fs", "tp"),
        P("fs", "tp"),
        P("fs", "tp"),
        P(),
        P("tp", "fs"),
        P(),
        P("fs", "tp"),
        P("fs", "tp"),
        P("tp", "fs"),
        P(),
    )
    out_specs = P(("grp", "fs"), None, "tp")
    body = ring_local if fits_ring(mesh) else plain_local

    return jax.shard_map(body, mesh=mesh, in_specs=in_specs, out_specs=out_specs, check_vma=False)
```

```python
import functools

import jax
import jax.numpy as jnp
from jax import lax
from jax.experimental import pallas as pl
from jax.experimental.pallas import tpu as pltpu
from jax.sharding import PartitionSpec as P


BF16 = jnp.bfloat16
F32 = jnp.float32
VMEM_LIMIT = 56 * 1024 * 1024


def rms_norm(values, gain):
    floats = values.astype(F32)
    scaled = floats * lax.rsqrt(jnp.mean(floats * floats, axis=-1, keepdims=True) + 1e-06)
    return (scaled * gain).astype(BF16)


def plain_local(
    tokens, mix_gain, gate_outer, gate_inner, value_weight, conv_taps, mix_out,
    ffn_gain, ffn_gate, ffn_up, ffn_down, out_gain,
):
    seq_count, length, columns = tokens.shape
    row_count = seq_count * length
    width = columns * lax.axis_size("tp")
    whole = lax.all_gather(tokens, "tp", axis=2, tiled=True).reshape(row_count, width)
    normed = rms_norm(whole, mix_gain)
    channels = gate_outer.shape[1]

    def project(left, weight):
        full = lax.all_gather(weight, "fs", axis=0, tiled=True)
        return jnp.dot(left, full, preferred_element_type=F32)

    outer = project(normed, gate_outer).astype(BF16)
    inner = project(normed, gate_inner).astype(BF16)
    values = project(normed, value_weight).astype(BF16)
    product = (inner.astype(F32) * values.astype(F32)).reshape(seq_count, length, channels)
    own_taps = lax.dynamic_slice_in_dim(conv_taps, lax.axis_index("tp") * channels, channels, 1)
    tap_count = conv_taps.shape[0]
    padded = jnp.pad(product, ((0, 0), (tap_count - 1, 0), (0, 0)))
    conv = jnp.zeros((seq_count, length, channels), F32)
    for offset in range(tap_count):
        conv = conv + own_taps[offset] * padded[:, offset : offset + length]
    gated = (outer.astype(F32) * conv.reshape(row_count, channels)).astype(BF16)
    mix_terms = jnp.dot(
        gated, lax.all_gather(mix_out, "fs", axis=1, tiled=True), preferred_element_type=F32
    )
    mix_full = lax.psum(mix_terms.astype(BF16), "tp").astype(F32)
    first_full = (whole.astype(F32) + mix_full).astype(BF16)
    first = lax.dynamic_slice_in_dim(first_full, lax.axis_index("tp") * columns, columns, 1)
    normed_ffn = rms_norm(first_full, ffn_gain)
    gate = project(normed_ffn, ffn_gate)
    upward = project(normed_ffn, ffn_up)
    hidden = (jax.nn.silu(gate) * upward).astype(BF16)
    down_terms = jnp.dot(
        hidden, lax.all_gather(ffn_down, "fs", axis=1, tiled=True), preferred_element_type=F32
    )
    down_summed = lax.psum_scatter(
        down_terms.astype(BF16), "tp", scatter_dimension=1, tiled=True
    ).astype(F32)
    second = first.astype(F32) + down_summed
    squares = lax.psum(jnp.sum(second * second, axis=1), "tp")
    factor = lax.rsqrt(squares / width + 1e-06)
    own_gain = lax.dynamic_slice_in_dim(out_gain, lax.axis_index("tp") * columns, columns, 0)
    result = second * factor[:, None] * own_gain
    return result.astype(BF16).reshape(seq_count, length, columns)


def dot(left, right):
    return jnp.dot(left, right, preferred_element_type=F32)


def norm_kernel(info, gain, b0, b1, b2, b3, out, *, width):
    q = info[2]
    blocks = [(b, h) for b in (b0, b1, b2, b3) for h in range(2)]
    squares = None
    for b, h in blocks:
        value = b[h].astype(F32)
        squares = value * value if squares is None else squares + value * value
    factor = lax.rsqrt(jnp.sum(squares, axis=-1, keepdims=True) / width + 1e-06)
    for i, (b, h) in enumerate(blocks):
        own = gain[(q ^ (i // 2)) * 2 + h]
        out[i] = (b[h].astype(F32) * factor * own).astype(BF16)


def call(kernel, info, operands, outs, flops):
    in_vmem = pl.BlockSpec(memory_space=pltpu.VMEM)
    moved = 2 * sum(o.size for o in operands)
    return pl.pallas_call(
        kernel,
        in_specs=[pl.BlockSpec(memory_space=pltpu.SMEM)] + [in_vmem] * len(operands),
        out_specs=[in_vmem] * len(outs),
        out_shape=[jax.ShapeDtypeStruct(shape, BF16) for shape in outs],
        cost_estimate=pl.CostEstimate(flops=flops, bytes_accessed=moved, transcendentals=0),
        compiler_params=pltpu.CompilerParams(vmem_limit_bytes=VMEM_LIMIT),
    )(info, *operands)


def norm_call(info, gain, blocks):
    _, rows, half = blocks[0].shape
    width = 8 * half
    kernel = functools.partial(norm_kernel, width=width)
    operands = [gain.reshape(8, 1, half), *blocks]
    return call(kernel, info, operands, [(8, rows, half)], 4000000)[0]


def place(info, step, direction, count):
    z, q = info[0], info[2]
    shard = lax.rem(z + (count - step if direction > 0 else step), count)
    return shard ^ q


def gathered(x, info, pieces, direction, count):
    g = info[1]
    spot = place(info, 0, direction, count)
    parts = [x[2 * spot], x[2 * spot + 1]]
    for step, swapped, _ in pieces:
        spot = place(info, step, direction, count)
        parts.append(x[2 * spot + (1 - g if swapped else g)])
    return jnp.concatenate(parts, axis=1)


def stacked(own, pieces, row, half, columns):
    rows = [own[:, columns]] + [piece[row : row + half, :] for _, _, piece in pieces]
    return jnp.concatenate(rows, axis=0)


def sort_out(keep, give, spot, part, value):
    value = value.astype(BF16)

    @pl.when(lax.rem(spot, 2) == 0)
    def _():
        keep[spot // 2, part] = value

    @pl.when(lax.rem(spot, 2) == 1)
    def _():
        give[spot // 2, part] = value


def mixer_kernel(*refs, count, length):
    info, taps, x, outer_own, inner_own, value_own, mix_own = refs[:7]
    steps = count - 1
    ahead, ahead_y = refs[7 : 7 + steps], refs[7 + steps : 7 + 2 * steps]
    back, back_y = refs[7 + 2 * steps : 7 + 3 * steps], refs[7 + 3 * steps : 7 + 4 * steps]
    keep, give = refs[-2:]
    half = x.shape[2]
    everything = slice(None)
    g = info[1]
    cw = [(k + 1, s, p) for s, group in ((False, ahead), (True, ahead_y)) for k, p in enumerate(group)]
    ccw = [(k + 1, s, p) for s, group in ((False, back), (True, back_y)) for k, p in enumerate(group)]
    left = gathered(x, info, cw, 1, count)
    inner = dot(left, stacked(inner_own, cw, 0, half, everything)).astype(BF16)
    values = dot(left, stacked(value_own, cw, half, half, everything)).astype(BF16)
    left = gathered(x, info, ccw, -1, count)
    outer = dot(left, stacked(outer_own, ccw, 0, half, everything)).astype(BF16)
    product = inner.astype(F32) * values.astype(F32)
    position = lax.broadcasted_iota(jnp.int32, product.shape, 0) % length
    tap_count = taps.shape[0]
    conv = jnp.zeros(product.shape, F32)
    channels = product.shape[1]
    own_taps = taps[:, pl.ds(pl.multiple_of(info[2] * channels, 128), channels)]
    for offset in range(tap_count):
        back_by = tap_count - 1 - offset
        if back_by:
            moved = pltpu.roll(product, back_by, axis=0)
            moved = jnp.where(position >= back_by, moved, 0.0)
        else:
            moved = product
        conv = conv + own_taps[offset][None, :] * moved
    gated = (outer.astype(F32) * conv).astype(BF16)

    own = dot(gated, mix_own[...])
    for h in range(2):
        sort_out(keep, give, place(info, 0, -1, count), h, own[:, h * half : (h + 1) * half])
    for step, swapped, piece in ccw:
        spot = place(info, step, -1, count)
        sort_out(keep, give, spot, 1 - g if swapped else g, dot(gated, piece[half:, :]))


def mixer_call(info, taps, x, owns, cw, cw_y, ccw, ccw_y, count, length):
    _, rows, half = x.shape
    kernel = functools.partial(mixer_kernel, count=count, length=length)
    operands = [taps, x, *owns, *cw, *cw_y, *ccw, *ccw_y]
    flops = 8 * rows * 8 * half * owns[0].shape[1]
    return call(kernel, info, operands, [(2, 2, rows, half)] * 2, flops)


def hidden_kernel(*refs, count, start, size):
    info, x, gate_own, up_own = refs[:4]
    steps = count - 1
    groups = [refs[4 + i * steps : 4 + (i + 1) * steps] for i in range(4)]
    out = refs[-1]
    columns = slice(start, start + size)
    cw = [(k + 1, i == 1, p) for i in (0, 1) for k, p in enumerate(groups[i])]
    ccw = [(k + 1, i == 3, p) for i in (2, 3) for k, p in enumerate(groups[i])]
    half = x.shape[2]
    gate = dot(gathered(x, info, cw, 1, count), stacked(gate_own, cw, 0, half, columns))
    upward = dot(gathered(x, info, ccw, -1, count), stacked(up_own, ccw, 0, half, columns))
    out[...] = (gate / (1.0 + jnp.exp(-gate)) * upward).astype(BF16)


def hidden_call(info, x, gate_own, up_own, cw, cw_y, ccw, ccw_y, count, start, size):
    _, rows, half = x.shape
    kernel = functools.partial(hidden_kernel, count=count, start=start, size=size)
    operands = [x, gate_own, up_own, *cw, *cw_y, *ccw, *ccw_y]
    return call(kernel, info, operands, [(rows, size)], 4 * rows * 8 * half * size)[0]


def down_early_kernel(*refs, count, split):
    info, left, right, own = refs[:4]
    steps = count - 2
    groups = [refs[4 + i * steps : 4 + (i + 1) * steps] for i in range(4)]
    keep, give = refs[-2:]
    g = info[1]
    rows, piece = keep.shape[-2:]

    def product(weight):
        return dot(left[...], weight[:split]) + dot(right[...], weight[split:])

    def store(step, direction, part, value):
        sort_out(keep, give, place(info, step, direction, count), part, value)

    value = product(own[...])
    for i in range(4):
        store(0, 1, i, value[:, i * piece : (i + 1) * piece])
    for direction, last, mine, other in ((1, 0, groups[0], groups[1]), (-1, 1, groups[2], groups[3])):
        value = product(jnp.concatenate([p[...] for k in range(steps) for p in (mine[k], other[k])], axis=1))
        for k in range(steps):
            at = 2 * k * piece
            store(k + 1, direction, 2 * g + last, value[:, at : at + piece])
            store(k + 1, direction, 2 * (1 - g) + last, value[:, at + piece : at + 2 * piece])
        for i in range(2):
            store(count - 1, direction, 2 * i + last, jnp.zeros((rows, piece), F32))


def down_late_kernel(info, left, right, cw, cw_y, ccw, ccw_y, out, *, count, split):
    g = info[1]
    piece = out.shape[-1]
    for direction, mine, other in ((1, cw, cw_y), (-1, ccw, ccw_y)):
        weight = jnp.concatenate([mine[...], other[...]], axis=1)
        value = dot(left[...], weight[:split]) + dot(right[...], weight[split:])
        spot = place(info, count - 1, direction, count) // 2
        out[spot, g] = value[:, :piece].astype(BF16)
        out[spot, 1 - g] = value[:, piece:].astype(BF16)


def ring_local(
    tokens, mix_gain, gate_outer, gate_inner, value_weight, conv_taps, mix_out,
    ffn_gain, ffn_gate, ffn_up, ffn_down, out_gain,
):
    count = lax.axis_size("fs")
    seq_count, length, columns = tokens.shape
    rows = seq_count * length
    half = columns // 2
    width = columns * lax.axis_size("tp")
    z, g, q = lax.axis_index("fs"), lax.axis_index("grp"), lax.axis_index("tp")
    info = jnp.stack([z, g, q]).astype(jnp.int32)

    ahead = [(i, (i + 1) % count) for i in range(count)]
    behind = [(d, s) for s, d in ahead]

    def ring(value, pairs):
        arrived, swapped = [], []
        for _ in range(1, count):
            value = lax.ppermute(value, "fs", pairs)
            arrived.append(value)
            swapped.append(lax.ppermute(value, "grp", [(0, 1), (1, 0)]))
        return arrived, swapped

    def mate(value):
        return lax.ppermute(value, "tp", [(i, i ^ 1) for i in range(4)])

    def across(value):
        return lax.ppermute(value, "tp", [(i, i ^ 2) for i in range(4)])

    def gather(own):
        other = across(own)
        return own, mate(own), other, mate(other)

    def rows_of(weight):
        return lax.dynamic_slice_in_dim(weight, g * half, half, 0)

    own_tokens = tokens.reshape(rows, 2, half).transpose(1, 0, 2)
    blocks = gather(own_tokens)

    mix_half = lax.dynamic_slice_in_dim(mix_out, g * half, half, 1)
    m_cw = ring(jnp.concatenate([rows_of(gate_inner), rows_of(value_weight)]), ahead)
    m_ccw = ring(jnp.concatenate([rows_of(gate_outer), mix_half]), behind)
    units = ffn_gate.shape[1]
    split = -(-units // 256) * 128
    gate_half, up_half = rows_of(ffn_gate), rows_of(ffn_up)
    g1 = ring(gate_half[:, :split], ahead)
    u1 = ring(up_half[:, :split], behind)
    g2 = ring(gate_half[:, split:], ahead)
    u2 = ring(up_half[:, split:], behind)
    down_half = lax.dynamic_slice_in_dim(ffn_down, g * half, half, 1)
    d_cw = ring(down_half[:, : half // 2], ahead)
    d_ccw = ring(down_half[:, half // 2 :], behind)

    def scatter(partial):
        met = partial[0].astype(F32) + mate(partial[1]).astype(F32)
        return met[0] + across(met[1].astype(BF16)).astype(F32)

    x = norm_call(info, mix_gain, blocks)
    owns = (gate_outer, gate_inner, value_weight, mix_out)
    partial = mixer_call(info, conv_taps, x, owns, *m_cw, *m_ccw, count, length)
    first = (own_tokens.astype(F32) + scatter(partial)).astype(BF16)
    blocks = gather(first)
    x = norm_call(info, ffn_gain, blocks)
    left = hidden_call(info, x, ffn_gate, ffn_up, *g1, *u1, count, 0, split)
    right = hidden_call(info, x, ffn_gate, ffn_up, *g2, *u2, count, split, units - split)
    flops = 2 * rows * units * width
    early = [left, right, ffn_down, *[p for ring_part in (*d_cw, *d_ccw) for p in ring_part[:-1]]]
    late = [left, right, *[ring_part[-1] for ring_part in (*d_cw, *d_ccw)]]
    split_by = {"count": count, "split": split}
    piece = (rows, half // 2)
    kernel = functools.partial(down_early_kernel, **split_by)
    partial = call(kernel, info, early, [(2, 4, *piece)] * 2, flops * 3 // 4)
    second = first.reshape(2, rows, 2, half // 2).transpose(0, 2, 1, 3).reshape(4, rows, half // 2)
    second = second.astype(F32) + scatter(partial)
    kernel = functools.partial(down_late_kernel, **split_by)
    rest = call(kernel, info, late, [(2, 2, *piece)], flops // 4)[0]

    takers = [[(s + 1) % 2 == i % 2 for i in range(4)] for s in range(count)]
    to_mate = [(4 * s + i, 4 * s + (i ^ 1)) for s in range(count) for i in range(4) if not takers[s][i]]
    to_other = [(4 * s + i, 4 * s + (i ^ 2)) for s in range(count) for i in range(4) if takers[s][i]]
    met = rest.astype(F32) + lax.ppermute(rest, ("fs", "tp"), to_mate).astype(F32)
    met = met[0] + lax.ppermute(met[1].astype(BF16), ("fs", "tp"), to_other).astype(F32)
    takes = lax.rem(z + 1 + q, 2) == 0
    parity = jnp.where(q == lax.rem(z + 1, count), 0, 1)
    mask = takes & (jnp.arange(2) == parity)
    late_part = jnp.where(mask[None, :, None, None], met[:, None], 0.0).reshape(second.shape)
    second = second + late_part
    squares = lax.psum(jnp.sum(second * second, axis=(0, 2)), "tp")
    factor = lax.rsqrt(squares / width + 1e-06)
    own_gain = lax.dynamic_slice_in_dim(out_gain, q * columns, columns, 0).reshape(4, 1, half // 2)
    result = (second * factor[None, :, None] * own_gain).astype(BF16)
    return result.transpose(1, 0, 2).reshape(seq_count, length, columns)


def fits_ring(mesh):
    shape = mesh.shape
    return shape["grp"] == 2 and shape["tp"] == 4 and shape["fs"] == 4


def solution(mesh):
    in_specs = (
        P(("grp", "fs"), None, "tp"),
        P(),
        P("fs", "tp"),
        P("fs", "tp"),
        P("fs", "tp"),
        P(),
        P("tp", "fs"),
        P(),
        P("fs", "tp"),
        P("fs", "tp"),
        P("tp", "fs"),
        P(),
    )
    out_specs = P(("grp", "fs"), None, "tp")
    ring = fits_ring(mesh)
    body = ring_local if ring else plain_local

    return jax.shard_map(body, mesh=mesh, in_specs=in_specs, out_specs=out_specs, check_vma=False)
```

```python
import functools

import jax
import jax.numpy as jnp
from jax import lax
from jax.experimental import pallas as pl
from jax.experimental.pallas import tpu as pltpu
from jax.sharding import PartitionSpec as P


BF16 = jnp.bfloat16
F32 = jnp.float32
VMEM_LIMIT = 20 * 1024 * 1024


def rms_norm(values, gain):
    floats = values.astype(F32)
    scaled = floats * lax.rsqrt(jnp.mean(floats * floats, axis=-1, keepdims=True) + 1e-06)
    return (scaled * gain).astype(BF16)


def plain_local(
    tokens, mix_gain, gate_outer, gate_inner, value_weight, conv_taps, mix_out,
    ffn_gain, ffn_gate, ffn_up, ffn_down, out_gain,
):
    seq_count, length, columns = tokens.shape
    row_count = seq_count * length
    width = columns * lax.axis_size("tp")
    whole = lax.all_gather(tokens, "tp", axis=2, tiled=True).reshape(row_count, width)
    normed = rms_norm(whole, mix_gain)
    channels = gate_outer.shape[1]

    def project(left, weight):
        full = lax.all_gather(weight, "fs", axis=0, tiled=True)
        return jnp.dot(left, full, preferred_element_type=F32)

    outer = project(normed, gate_outer).astype(BF16)
    inner = project(normed, gate_inner).astype(BF16)
    values = project(normed, value_weight).astype(BF16)
    product = (inner.astype(F32) * values.astype(F32)).reshape(seq_count, length, channels)
    own_taps = lax.dynamic_slice_in_dim(conv_taps, lax.axis_index("tp") * channels, channels, 1)
    tap_count = conv_taps.shape[0]
    padded = jnp.pad(product, ((0, 0), (tap_count - 1, 0), (0, 0)))
    conv = jnp.zeros((seq_count, length, channels), F32)
    for offset in range(tap_count):
        conv = conv + own_taps[offset] * padded[:, offset : offset + length]
    gated = (outer.astype(F32) * conv.reshape(row_count, channels)).astype(BF16)
    mix_terms = jnp.dot(
        gated, lax.all_gather(mix_out, "fs", axis=1, tiled=True), preferred_element_type=F32
    )
    mix_full = lax.psum(mix_terms.astype(BF16), "tp").astype(F32)
    first_full = (whole.astype(F32) + mix_full).astype(BF16)
    first = lax.dynamic_slice_in_dim(first_full, lax.axis_index("tp") * columns, columns, 1)
    normed_ffn = rms_norm(first_full, ffn_gain)
    gate = project(normed_ffn, ffn_gate)
    upward = project(normed_ffn, ffn_up)
    hidden = (jax.nn.silu(gate) * upward).astype(BF16)
    down_terms = jnp.dot(
        hidden, lax.all_gather(ffn_down, "fs", axis=1, tiled=True), preferred_element_type=F32
    )
    down_summed = lax.psum_scatter(
        down_terms.astype(BF16), "tp", scatter_dimension=1, tiled=True
    ).astype(F32)
    second = first.astype(F32) + down_summed
    squares = lax.psum(jnp.sum(second * second, axis=1), "tp")
    factor = lax.rsqrt(squares / width + 1e-06)
    own_gain = lax.dynamic_slice_in_dim(out_gain, lax.axis_index("tp") * columns, columns, 0)
    result = second * factor[:, None] * own_gain
    return result.astype(BF16).reshape(seq_count, length, columns)


def dot(left, right):
    return jnp.dot(left, right, preferred_element_type=F32)


def norm_kernel(info, gain, b0, b1, b2, b3, out, *, width):
    q = info[2]
    blocks = [(b, h) for b in (b0, b1, b2, b3) for h in range(2)]
    squares = None
    for b, h in blocks:
        value = b[h].astype(F32)
        squares = value * value if squares is None else squares + value * value
    factor = lax.rsqrt(jnp.sum(squares, axis=-1, keepdims=True) / width + 1e-06)
    for i, (b, h) in enumerate(blocks):
        own = gain[(q ^ (i // 2)) * 2 + h]
        out[i] = (b[h].astype(F32) * factor * own).astype(BF16)


def call(kernel, info, operands, outs, flops):
    in_vmem = pl.BlockSpec(memory_space=pltpu.VMEM)
    moved = 2 * sum(o.size for o in operands)
    return pl.pallas_call(
        kernel,
        in_specs=[pl.BlockSpec(memory_space=pltpu.SMEM)] + [in_vmem] * len(operands),
        out_specs=[in_vmem] * len(outs),
        out_shape=[jax.ShapeDtypeStruct(shape, BF16) for shape in outs],
        cost_estimate=pl.CostEstimate(flops=flops, bytes_accessed=moved, transcendentals=0),
        compiler_params=pltpu.CompilerParams(vmem_limit_bytes=VMEM_LIMIT),
    )(info, *operands)


def norm_call(info, gain, blocks):
    _, rows, half = blocks[0].shape
    width = 8 * half
    kernel = functools.partial(norm_kernel, width=width)
    operands = [gain.reshape(8, 1, half), *blocks]
    return call(kernel, info, operands, [(8, rows, half)], 4000000)[0]


def place(info, step, direction, count):
    z, q = info[0], info[2]
    shard = lax.rem(z + (count - step if direction > 0 else step), count)
    return shard ^ q


def gathered(x, info, pieces, direction, count):
    g = info[1]
    spot = place(info, 0, direction, count)
    parts = [x[2 * spot], x[2 * spot + 1]]
    for step, swapped, _ in pieces:
        spot = place(info, step, direction, count)
        parts.append(x[2 * spot + (1 - g if swapped else g)])
    return jnp.concatenate(parts, axis=1)


def stacked(own, pieces, row, half, columns):
    rows = [own[:, columns]] + [piece[row : row + half, :] for _, _, piece in pieces]
    return jnp.concatenate(rows, axis=0)


def sort_out(keep, give, spot, part, value):
    value = value.astype(BF16)

    @pl.when(lax.rem(spot, 2) == 0)
    def _():
        keep[spot // 2, part] = value

    @pl.when(lax.rem(spot, 2) == 1)
    def _():
        give[spot // 2, part] = value


def mixer_kernel(*refs, count, length):
    info, taps, x, outer_own, inner_own, value_own, mix_own = refs[:7]
    steps = count - 1
    ahead, ahead_y = refs[7 : 7 + steps], refs[7 + steps : 7 + 2 * steps]
    back, back_y = refs[7 + 2 * steps : 7 + 3 * steps], refs[7 + 3 * steps : 7 + 4 * steps]
    keep, give = refs[-2:]
    half = x.shape[2]
    everything = slice(None)
    g = info[1]
    cw = [(k + 1, s, p) for s, group in ((False, ahead), (True, ahead_y)) for k, p in enumerate(group)]
    ccw = [(k + 1, s, p) for s, group in ((False, back), (True, back_y)) for k, p in enumerate(group)]
    left = gathered(x, info, cw, 1, count)
    inner = dot(left, stacked(inner_own, cw, 0, half, everything)).astype(BF16)
    values = dot(left, stacked(value_own, cw, half, half, everything)).astype(BF16)
    left = gathered(x, info, ccw, -1, count)
    outer = dot(left, stacked(outer_own, ccw, 0, half, everything)).astype(BF16)
    product = inner.astype(F32) * values.astype(F32)
    position = lax.broadcasted_iota(jnp.int32, product.shape, 0) % length
    tap_count = taps.shape[0]
    conv = jnp.zeros(product.shape, F32)
    channels = product.shape[1]
    own_taps = taps[:, pl.ds(pl.multiple_of(info[2] * channels, 128), channels)]
    for offset in range(tap_count):
        back_by = tap_count - 1 - offset
        if back_by:
            moved = pltpu.roll(product, back_by, axis=0)
            moved = jnp.where(position >= back_by, moved, 0.0)
        else:
            moved = product
        conv = conv + own_taps[offset][None, :] * moved
    gated = (outer.astype(F32) * conv).astype(BF16)

    own = dot(gated, mix_own[...])
    for h in range(2):
        sort_out(keep, give, place(info, 0, -1, count), h, own[:, h * half : (h + 1) * half])
    for step, swapped, piece in ccw:
        spot = place(info, step, -1, count)
        sort_out(keep, give, spot, 1 - g if swapped else g, dot(gated, piece[half:, :]))


def mixer_call(info, taps, x, owns, cw, cw_y, ccw, ccw_y, count, length):
    _, rows, half = x.shape
    kernel = functools.partial(mixer_kernel, count=count, length=length)
    operands = [taps, x, *owns, *cw, *cw_y, *ccw, *ccw_y]
    flops = 8 * rows * 8 * half * owns[0].shape[1]
    return call(kernel, info, operands, [(2, 2, rows, half)] * 2, flops)


def hidden_kernel(*refs, count, start, size):
    info, x, gate_own, up_own = refs[:4]
    steps = count - 1
    groups = [refs[4 + i * steps : 4 + (i + 1) * steps] for i in range(4)]
    out = refs[-1]
    columns = slice(start, start + size)
    cw = [(k + 1, i == 1, p) for i in (0, 1) for k, p in enumerate(groups[i])]
    ccw = [(k + 1, i == 3, p) for i in (2, 3) for k, p in enumerate(groups[i])]
    half = x.shape[2]
    gate = dot(gathered(x, info, cw, 1, count), stacked(gate_own, cw, 0, half, columns))
    upward = dot(gathered(x, info, ccw, -1, count), stacked(up_own, ccw, 0, half, columns))
    out[...] = (gate / (1.0 + jnp.exp(-gate)) * upward).astype(BF16)


def hidden_call(info, x, gate_own, up_own, cw, cw_y, ccw, ccw_y, count, start, size):
    _, rows, half = x.shape
    kernel = functools.partial(hidden_kernel, count=count, start=start, size=size)
    operands = [x, gate_own, up_own, *cw, *cw_y, *ccw, *ccw_y]
    return call(kernel, info, operands, [(rows, size)], 4 * rows * 8 * half * size)[0]


def down_early_kernel(*refs, count, split):
    info, left, right, own = refs[:4]
    steps = count - 2
    groups = [refs[4 + i * steps : 4 + (i + 1) * steps] for i in range(4)]
    keep, give = refs[-2:]
    g = info[1]
    rows, piece = keep.shape[-2:]

    def product(weight):
        return dot(left[...], weight[:split]) + dot(right[...], weight[split:])

    def store(step, direction, part, value):
        sort_out(keep, give, place(info, step, direction, count), part, value)

    value = product(own[...])
    for i in range(4):
        store(0, 1, i, value[:, i * piece : (i + 1) * piece])
    for direction, last, mine, other in ((1, 0, groups[0], groups[1]), (-1, 1, groups[2], groups[3])):
        value = product(jnp.concatenate([p[...] for k in range(steps) for p in (mine[k], other[k])], axis=1))
        for k in range(steps):
            at = 2 * k * piece
            store(k + 1, direction, 2 * g + last, value[:, at : at + piece])
            store(k + 1, direction, 2 * (1 - g) + last, value[:, at + piece : at + 2 * piece])
        for i in range(2):
            store(count - 1, direction, 2 * i + last, jnp.zeros((rows, piece), F32))


def down_late_kernel(info, left, right, cw, cw_y, ccw, ccw_y, near, far, *, count, split):
    g = info[1]
    piece = near.shape[-1]
    weight = jnp.concatenate([p[...] for p in (cw, cw_y, ccw, ccw_y)], axis=1)
    value = (dot(left[...], weight[:split]) + dot(right[...], weight[split:])).astype(BF16)
    for i, direction in enumerate((1, -1)):
        spot = place(info, count - 1, direction, count) // 2
        for at, target in enumerate((near, far)):

            @pl.when(spot == at)
            def _():
                target[g] = value[:, 2 * i * piece : (2 * i + 1) * piece]
                target[1 - g] = value[:, (2 * i + 1) * piece : (2 * i + 2) * piece]


def close_kernel(squares, second, gain, out, *, width):
    rows, piece = second.shape[1:]
    factor = lax.rsqrt(squares[...] / width + 1e-06)
    factor = jnp.broadcast_to(factor, (piece, rows)).T
    for p in range(second.shape[0]):
        out[:, p * piece : (p + 1) * piece] = (second[p] * factor * gain[p]).astype(BF16)


def ring_local(
    tokens, mix_gain, gate_outer, gate_inner, value_weight, conv_taps, mix_out,
    ffn_gain, ffn_gate, ffn_up, ffn_down, out_gain,
):
    count = lax.axis_size("fs")
    seq_count, length, columns = tokens.shape
    rows = seq_count * length
    half = columns // 2
    width = columns * lax.axis_size("tp")
    z, g, q = lax.axis_index("fs"), lax.axis_index("grp"), lax.axis_index("tp")
    info = jnp.stack([z, g, q]).astype(jnp.int32)

    ahead = [(i, (i + 1) % count) for i in range(count)]
    behind = [(d, s) for s, d in ahead]

    def ring(value, pairs):
        arrived, swapped = [], []
        for _ in range(1, count):
            value = lax.ppermute(value, "fs", pairs)
            arrived.append(value)
            swapped.append(lax.ppermute(value, "grp", [(0, 1), (1, 0)]))
        return arrived, swapped

    def mate(value):
        return lax.ppermute(value, "tp", [(i, i ^ 1) for i in range(4)])

    def across(value):
        return lax.ppermute(value, "tp", [(i, i ^ 2) for i in range(4)])

    def gather(own):
        other = across(own)
        return own, mate(own), other, mate(other)

    def rows_of(weight):
        return lax.dynamic_slice_in_dim(weight, g * half, half, 0)

    own_tokens = tokens.reshape(rows, 2, half).transpose(1, 0, 2)
    blocks = gather(own_tokens)

    mix_half = lax.dynamic_slice_in_dim(mix_out, g * half, half, 1)
    m_cw = ring(jnp.concatenate([rows_of(gate_inner), rows_of(value_weight)]), ahead)
    m_ccw = ring(jnp.concatenate([rows_of(gate_outer), mix_half]), behind)
    units = ffn_gate.shape[1]
    split = -(-units // 256) * 128
    gate_half, up_half = rows_of(ffn_gate), rows_of(ffn_up)
    g1 = ring(gate_half[:, :split], ahead)
    u1 = ring(up_half[:, :split], behind)
    g2 = ring(gate_half[:, split:], ahead)
    u2 = ring(up_half[:, split:], behind)
    down_half = lax.dynamic_slice_in_dim(ffn_down, g * half, half, 1)
    d_cw = ring(down_half[:, : half // 2], ahead)
    d_ccw = ring(down_half[:, half // 2 :], behind)

    def scatter(partial):
        met = partial[0].astype(F32) + mate(partial[1]).astype(F32)
        return met[0] + across(met[1].astype(BF16)).astype(F32)

    x = norm_call(info, mix_gain, blocks)
    owns = (gate_outer, gate_inner, value_weight, mix_out)
    partial = mixer_call(info, conv_taps, x, owns, *m_cw, *m_ccw, count, length)
    first = (own_tokens.astype(F32) + scatter(partial)).astype(BF16)
    blocks = gather(first)
    x = norm_call(info, ffn_gain, blocks)
    left = hidden_call(info, x, ffn_gate, ffn_up, *g1, *u1, count, 0, split)
    right = hidden_call(info, x, ffn_gate, ffn_up, *g2, *u2, count, split, units - split)
    flops = 2 * rows * units * width
    early = [left, right, ffn_down, *[p for ring_part in (*d_cw, *d_ccw) for p in ring_part[:-1]]]
    late = [left, right, *[ring_part[-1] for ring_part in (*d_cw, *d_ccw)]]
    split_by = {"count": count, "split": split}
    piece = (rows, half // 2)
    kernel = functools.partial(down_early_kernel, **split_by)
    partial = call(kernel, info, early, [(2, 4, *piece)] * 2, flops * 3 // 4)
    second = first.reshape(2, rows, 2, half // 2).transpose(0, 2, 1, 3).reshape(4, rows, half // 2)
    second = second.astype(F32) + scatter(partial)
    kernel = functools.partial(down_late_kernel, **split_by)
    near, far = call(kernel, info, late, [(2, *piece)] * 2, flops // 4)

    both = [(s, i) for s in range(count) for i in range(4)]
    takers = [(s, i) for s, i in both if (s + 1) % 2 == i % 2]
    others = [(s, i) for s, i in both if (s + 1) % 2 != i % 2]

    def late_send(value, senders, flip):
        pairs = [(4 * s + i, 4 * s + (i ^ flip)) for s, i in senders]
        return lax.ppermute(value, ("fs", "tp"), pairs).astype(F32)

    met = late_send(far, takers, 2) + late_send(far, others, 3)
    met = met + late_send(near, others, 1) + near.astype(F32)
    takes = lax.rem(z + 1 + q, 2) == 0
    parity = jnp.where(q == lax.rem(z + 1, count), 0, 1)
    mask = takes & (jnp.arange(2) == parity)
    late_part = jnp.where(mask[None, :, None, None], met[:, None], 0.0).reshape(second.shape)
    second = second + late_part
    squares = lax.psum(jnp.sum(second * second, axis=(0, 2)), "tp")
    own_gain = lax.dynamic_slice_in_dim(out_gain, q * columns, columns, 0).reshape(4, 1, half // 2)
    in_vmem = pl.BlockSpec(memory_space=pltpu.VMEM)
    result = pl.pallas_call(
        functools.partial(close_kernel, width=width),
        in_specs=[in_vmem] * 3,
        out_specs=in_vmem,
        out_shape=jax.ShapeDtypeStruct((rows, columns), BF16),
        compiler_params=pltpu.CompilerParams(vmem_limit_bytes=VMEM_LIMIT),
        name="close",
    )(squares.reshape(1, rows), second, own_gain)
    return result.reshape(seq_count, length, columns)


def fits_ring(mesh):
    shape = mesh.shape
    return shape["grp"] == 2 and shape["tp"] == 4 and shape["fs"] == 4


def solution(mesh):
    in_specs = (
        P(("grp", "fs"), None, "tp"),
        P(),
        P("fs", "tp"),
        P("fs", "tp"),
        P("fs", "tp"),
        P(),
        P("tp", "fs"),
        P(),
        P("fs", "tp"),
        P("fs", "tp"),
        P("tp", "fs"),
        P(),
    )
    out_specs = P(("grp", "fs"), None, "tp")
    ring = fits_ring(mesh)
    body = ring_local if ring else plain_local

    return jax.shard_map(body, mesh=mesh, in_specs=in_specs, out_specs=out_specs, check_vma=False)
```

```python
import functools

import jax
import jax.numpy as jnp
from jax import lax
from jax.experimental import pallas as pl
from jax.experimental.pallas import tpu as pltpu
from jax.sharding import PartitionSpec as P


BF16 = jnp.bfloat16
F32 = jnp.float32
VMEM_LIMIT = 20 * 1024 * 1024


def rms_norm(values, gain):
    floats = values.astype(F32)
    scaled = floats * lax.rsqrt(jnp.mean(floats * floats, axis=-1, keepdims=True) + 1e-06)
    return (scaled * gain).astype(BF16)


def plain_local(
    tokens, mix_gain, gate_outer, gate_inner, value_weight, conv_taps, mix_out,
    ffn_gain, ffn_gate, ffn_up, ffn_down, out_gain,
):
    seq_count, length, columns = tokens.shape
    row_count = seq_count * length
    width = columns * lax.axis_size("tp")
    whole = lax.all_gather(tokens, "tp", axis=2, tiled=True).reshape(row_count, width)
    normed = rms_norm(whole, mix_gain)
    channels = gate_outer.shape[1]

    def project(left, weight):
        full = lax.all_gather(weight, "fs", axis=0, tiled=True)
        return jnp.dot(left, full, preferred_element_type=F32)

    outer = project(normed, gate_outer).astype(BF16)
    inner = project(normed, gate_inner).astype(BF16)
    values = project(normed, value_weight).astype(BF16)
    product = (inner.astype(F32) * values.astype(F32)).reshape(seq_count, length, channels)
    own_taps = lax.dynamic_slice_in_dim(conv_taps, lax.axis_index("tp") * channels, channels, 1)
    tap_count = conv_taps.shape[0]
    padded = jnp.pad(product, ((0, 0), (tap_count - 1, 0), (0, 0)))
    conv = jnp.zeros((seq_count, length, channels), F32)
    for offset in range(tap_count):
        conv = conv + own_taps[offset] * padded[:, offset : offset + length]
    gated = (outer.astype(F32) * conv.reshape(row_count, channels)).astype(BF16)
    mix_terms = jnp.dot(
        gated, lax.all_gather(mix_out, "fs", axis=1, tiled=True), preferred_element_type=F32
    )
    mix_full = lax.psum(mix_terms.astype(BF16), "tp").astype(F32)
    first_full = (whole.astype(F32) + mix_full).astype(BF16)
    first = lax.dynamic_slice_in_dim(first_full, lax.axis_index("tp") * columns, columns, 1)
    normed_ffn = rms_norm(first_full, ffn_gain)
    gate = project(normed_ffn, ffn_gate)
    upward = project(normed_ffn, ffn_up)
    hidden = (jax.nn.silu(gate) * upward).astype(BF16)
    down_terms = jnp.dot(
        hidden, lax.all_gather(ffn_down, "fs", axis=1, tiled=True), preferred_element_type=F32
    )
    down_summed = lax.psum_scatter(
        down_terms.astype(BF16), "tp", scatter_dimension=1, tiled=True
    ).astype(F32)
    second = first.astype(F32) + down_summed
    squares = lax.psum(jnp.sum(second * second, axis=1), "tp")
    factor = lax.rsqrt(squares / width + 1e-06)
    own_gain = lax.dynamic_slice_in_dim(out_gain, lax.axis_index("tp") * columns, columns, 0)
    result = second * factor[:, None] * own_gain
    return result.astype(BF16).reshape(seq_count, length, columns)


def dot(left, right):
    return jnp.dot(left, right, preferred_element_type=F32)


def norm_kernel(info, gain, b0, b1, b2, b3, out, *, width):
    q = info[2]
    blocks = [(b, h) for b in (b0, b1, b2, b3) for h in range(2)]
    squares = None
    for b, h in blocks:
        value = b[h].astype(F32)
        squares = value * value if squares is None else squares + value * value
    factor = lax.rsqrt(jnp.sum(squares, axis=-1, keepdims=True) / width + 1e-06)
    for i, (b, h) in enumerate(blocks):
        own = gain[(q ^ (i // 2)) * 2 + h]
        out[i] = (b[h].astype(F32) * factor * own).astype(BF16)


def call(kernel, info, operands, outs, flops):
    in_vmem = pl.BlockSpec(memory_space=pltpu.VMEM)
    moved = 2 * sum(o.size for o in operands)
    return pl.pallas_call(
        kernel,
        in_specs=[pl.BlockSpec(memory_space=pltpu.SMEM)] + [in_vmem] * len(operands),
        out_specs=[in_vmem] * len(outs),
        out_shape=[jax.ShapeDtypeStruct(shape, BF16) for shape in outs],
        cost_estimate=pl.CostEstimate(flops=flops, bytes_accessed=moved, transcendentals=0),
        compiler_params=pltpu.CompilerParams(vmem_limit_bytes=VMEM_LIMIT),
    )(info, *operands)


def norm_call(info, gain, blocks):
    _, rows, half = blocks[0].shape
    width = 8 * half
    kernel = functools.partial(norm_kernel, width=width)
    operands = [gain.reshape(8, 1, half), *blocks]
    return call(kernel, info, operands, [(8, rows, half)], 4000000)[0]


def place(info, step, direction, count):
    z, q = info[0], info[2]
    shard = lax.rem(z + (count - step if direction > 0 else step), count)
    return shard ^ q


def gathered(x, info, pieces, direction, count):
    g = info[1]
    spot = place(info, 0, direction, count)
    parts = [x[2 * spot], x[2 * spot + 1]]
    for step, swapped, _ in pieces:
        spot = place(info, step, direction, count)
        parts.append(x[2 * spot + (1 - g if swapped else g)])
    return jnp.concatenate(parts, axis=1)


def stacked(own, pieces, row, half, columns):
    rows = [own[:, columns]] + [piece[row : row + half, :] for _, _, piece in pieces]
    return jnp.concatenate(rows, axis=0)


def sort_out(keep, give, spot, part, value):
    value = value.astype(BF16)

    @pl.when(lax.rem(spot, 2) == 0)
    def _():
        keep[spot // 2, part] = value

    @pl.when(lax.rem(spot, 2) == 1)
    def _():
        give[spot // 2, part] = value


def mixer_kernel(*refs, count, length):
    info, taps, x, outer_own, inner_own, value_own, mix_own = refs[:7]
    steps = count - 1
    ahead, ahead_y = refs[7 : 7 + steps], refs[7 + steps : 7 + 2 * steps]
    back, back_y = refs[7 + 2 * steps : 7 + 3 * steps], refs[7 + 3 * steps : 7 + 4 * steps]
    keep, give = refs[-2:]
    half = x.shape[2]
    everything = slice(None)
    g = info[1]
    cw = [(k + 1, s, p) for s, group in ((False, ahead), (True, ahead_y)) for k, p in enumerate(group)]
    ccw = [(k + 1, s, p) for s, group in ((False, back), (True, back_y)) for k, p in enumerate(group)]
    left = gathered(x, info, cw, 1, count)
    inner = dot(left, stacked(inner_own, cw, 0, half, everything)).astype(BF16)
    values = dot(left, stacked(value_own, cw, half, half, everything)).astype(BF16)
    left = gathered(x, info, ccw, -1, count)
    outer = dot(left, stacked(outer_own, ccw, 0, half, everything)).astype(BF16)
    product = inner.astype(F32) * values.astype(F32)
    position = lax.broadcasted_iota(jnp.int32, product.shape, 0) % length
    tap_count = taps.shape[0]
    conv = jnp.zeros(product.shape, F32)
    channels = product.shape[1]
    own_taps = taps[:, pl.ds(pl.multiple_of(info[2] * channels, 128), channels)]
    for offset in range(tap_count):
        back_by = tap_count - 1 - offset
        if back_by:
            moved = pltpu.roll(product, back_by, axis=0)
            moved = jnp.where(position >= back_by, moved, 0.0)
        else:
            moved = product
        conv = conv + own_taps[offset][None, :] * moved
    gated = (outer.astype(F32) * conv).astype(BF16)

    own = dot(gated, mix_own[...])
    for h in range(2):
        sort_out(keep, give, place(info, 0, -1, count), h, own[:, h * half : (h + 1) * half])
    for step, swapped, piece in ccw:
        spot = place(info, step, -1, count)
        sort_out(keep, give, spot, 1 - g if swapped else g, dot(gated, piece[half:, :]))


def mixer_call(info, taps, x, owns, cw, cw_y, ccw, ccw_y, count, length):
    _, rows, half = x.shape
    kernel = functools.partial(mixer_kernel, count=count, length=length)
    operands = [taps, x, *owns, *cw, *cw_y, *ccw, *ccw_y]
    flops = 8 * rows * 8 * half * owns[0].shape[1]
    return call(kernel, info, operands, [(2, 2, rows, half)] * 2, flops)


def hidden_kernel(*refs, count, start, size):
    info, x, gate_own, up_own = refs[:4]
    steps = count - 1
    groups = [refs[4 + i * steps : 4 + (i + 1) * steps] for i in range(4)]
    out = refs[-1]
    columns = slice(start, start + size)
    cw = [(k + 1, i == 1, p) for i in (0, 1) for k, p in enumerate(groups[i])]
    ccw = [(k + 1, i == 3, p) for i in (2, 3) for k, p in enumerate(groups[i])]
    half = x.shape[2]
    gate = dot(gathered(x, info, cw, 1, count), stacked(gate_own, cw, 0, half, columns))
    upward = dot(gathered(x, info, ccw, -1, count), stacked(up_own, ccw, 0, half, columns))
    out[...] = (gate / (1.0 + jnp.exp(-gate)) * upward).astype(BF16)


def hidden_call(info, x, gate_own, up_own, cw, cw_y, ccw, ccw_y, count, start, size):
    _, rows, half = x.shape
    kernel = functools.partial(hidden_kernel, count=count, start=start, size=size)
    operands = [x, gate_own, up_own, *cw, *cw_y, *ccw, *ccw_y]
    return call(kernel, info, operands, [(rows, size)], 4 * rows * 8 * half * size)[0]


def split_refs(refs, steps):
    return [refs[i * steps : (i + 1) * steps] for i in range(4)]


def down_product(left, right, weight, split):
    return dot(left[...], weight[:split]) + dot(right[...], weight[split:])


def down_first_kernel(info, left, right, own, cw, cw_y, ccw, ccw_y, keep, give, *, count, split):
    g = info[1]
    rows, piece = keep.shape[-2:]

    def store(step, direction, part, value):
        sort_out(keep, give, place(info, step, direction, count), part, value)

    value = down_product(left, right, own, split)
    for i in range(4):
        store(0, 1, i, value[:, i * piece : (i + 1) * piece])
    weight = jnp.concatenate([p[...] for p in (cw, cw_y, ccw, ccw_y)], axis=1)
    value = down_product(left, right, weight, split)
    for last, direction in enumerate((1, -1)):
        at = 2 * last * piece
        store(1, direction, 2 * g + last, value[:, at : at + piece])
        store(1, direction, 2 * (1 - g) + last, value[:, at + piece : at + 2 * piece])
        for i in range(2):
            store(count - 1, direction, 2 * i + last, jnp.zeros((rows, piece), F32))


def down_next_kernel(*refs, count, split):
    info, left, right, keep_in, give_in = refs[:5]
    steps = count - 3
    groups = split_refs(refs[5 : 5 + 4 * steps], steps)
    keep, give = refs[-2:]
    g = info[1]
    piece = keep.shape[-1]
    keep[...] = keep_in[...]
    give[...] = give_in[...]
    for k in range(steps):
        weight = jnp.concatenate([group[k][...] for group in groups], axis=1)
        value = down_product(left, right, weight, split)
        for last, direction in enumerate((1, -1)):
            at = 2 * last * piece
            spot = place(info, k + 2, direction, count)
            sort_out(keep, give, spot, 2 * g + last, value[:, at : at + piece])
            sort_out(keep, give, spot, 2 * (1 - g) + last, value[:, at + piece : at + 2 * piece])


def down_late_kernel(info, left, right, cw, cw_y, ccw, ccw_y, out, *, count, split):
    g = info[1]
    piece = out.shape[-1]
    weight = jnp.concatenate([p[...] for p in (cw, cw_y, ccw, ccw_y)], axis=1)
    value = down_product(left, right, weight, split).astype(BF16)
    for i, direction in enumerate((1, -1)):
        spot = place(info, count - 1, direction, count) // 2
        out[spot, g] = value[:, 2 * i * piece : (2 * i + 1) * piece]
        out[spot, 1 - g] = value[:, (2 * i + 1) * piece : (2 * i + 2) * piece]


def close_kernel(squares, second, gain, out, *, width):
    rows, piece = second.shape[1:]
    factor = lax.rsqrt(squares[...] / width + 1e-06)
    factor = jnp.broadcast_to(factor, (piece, rows)).T
    for p in range(second.shape[0]):
        out[:, p * piece : (p + 1) * piece] = (second[p] * factor * gain[p]).astype(BF16)


def ring_local(
    tokens, mix_gain, gate_outer, gate_inner, value_weight, conv_taps, mix_out,
    ffn_gain, ffn_gate, ffn_up, ffn_down, out_gain,
):
    count = lax.axis_size("fs")
    seq_count, length, columns = tokens.shape
    rows = seq_count * length
    half = columns // 2
    width = columns * lax.axis_size("tp")
    z, g, q = lax.axis_index("fs"), lax.axis_index("grp"), lax.axis_index("tp")
    info = jnp.stack([z, g, q]).astype(jnp.int32)

    ahead = [(i, (i + 1) % count) for i in range(count)]
    behind = [(d, s) for s, d in ahead]

    def ring(value, pairs):
        arrived, swapped = [], []
        for _ in range(1, count):
            value = lax.ppermute(value, "fs", pairs)
            arrived.append(value)
            swapped.append(lax.ppermute(value, "grp", [(0, 1), (1, 0)]))
        return arrived, swapped

    def mate(value):
        return lax.ppermute(value, "tp", [(i, i ^ 1) for i in range(4)])

    def across(value):
        return lax.ppermute(value, "tp", [(i, i ^ 2) for i in range(4)])

    def gather(own):
        other = across(own)
        return own, mate(own), other, mate(other)

    def rows_of(weight):
        return lax.dynamic_slice_in_dim(weight, g * half, half, 0)

    own_tokens = tokens.reshape(rows, 2, half).transpose(1, 0, 2)
    blocks = gather(own_tokens)

    mix_half = lax.dynamic_slice_in_dim(mix_out, g * half, half, 1)
    m_cw = ring(jnp.concatenate([rows_of(gate_inner), rows_of(value_weight)]), ahead)
    m_ccw = ring(jnp.concatenate([rows_of(gate_outer), mix_half]), behind)
    units = ffn_gate.shape[1]
    split = -(-units // 256) * 128
    gate_half, up_half = rows_of(ffn_gate), rows_of(ffn_up)
    g1 = ring(gate_half[:, :split], ahead)
    u1 = ring(up_half[:, :split], behind)
    g2 = ring(gate_half[:, split:], ahead)
    u2 = ring(up_half[:, split:], behind)
    down_half = lax.dynamic_slice_in_dim(ffn_down, g * half, half, 1)
    d_cw = ring(down_half[:, : half // 2], ahead)
    d_ccw = ring(down_half[:, half // 2 :], behind)

    def scatter(partial):
        keep, got = partial[0], mate(partial[1])
        far = (keep[1].astype(F32) + got[1].astype(F32)).astype(BF16)
        far = lax.optimization_barrier(far)
        near = keep[0].astype(F32) + got[0].astype(F32)
        return near, across(far).astype(F32)

    x = norm_call(info, mix_gain, blocks)
    own_gain = lax.dynamic_slice_in_dim(out_gain, q * columns, columns, 0).reshape(4, 1, half // 2)
    x, own_gain = lax.optimization_barrier((x, own_gain))
    owns = (gate_outer, gate_inner, value_weight, mix_out)
    partial = mixer_call(info, conv_taps, x, owns, *m_cw, *m_ccw, count, length)
    near, other = scatter(partial)
    first = (own_tokens.astype(F32) + (near + other)).astype(BF16)
    blocks = gather(first)
    x = norm_call(info, ffn_gain, blocks)
    left = hidden_call(info, x, ffn_gate, ffn_up, *g1, *u1, count, 0, split)
    right = hidden_call(info, x, ffn_gate, ffn_up, *g2, *u2, count, split, units - split)
    flops = 2 * rows * units * width
    rings = (*d_cw, *d_ccw)
    split_by = {"count": count, "split": split}
    piece = (rows, half // 2)
    kernel = functools.partial(down_first_kernel, **split_by)
    operands = [left, right, ffn_down, *[ring_part[0] for ring_part in rings]]
    partial = call(kernel, info, operands, [(2, 4, *piece)] * 2, flops // 2)
    kernel = functools.partial(down_next_kernel, **split_by)
    operands = [left, right, *partial, *[p for ring_part in rings for p in ring_part[1:-1]]]
    partial = call(kernel, info, operands, [(2, 4, *piece)] * 2, flops // 4)
    second = first.reshape(2, rows, 2, half // 2).transpose(0, 2, 1, 3).reshape(4, rows, half // 2)
    near, other = scatter(partial)
    second = lax.optimization_barrier(second.astype(F32) + near)
    kernel = functools.partial(down_late_kernel, **split_by)
    late = [left, right, *[ring_part[-1] for ring_part in rings]]
    rest = call(kernel, info, late, [(2, 2, *piece)], flops // 4)[0]

    pairs = [(s, i) for s in range(count) for i in range(4)]
    to_mate = [(4 * s + i, 4 * s + (i ^ 1)) for s, i in pairs if (s + 1) % 2 != i % 2]
    to_other = [(4 * s + i, 4 * s + (i ^ 2)) for s, i in pairs if (s + 1) % 2 == i % 2]
    got = lax.ppermute(rest, ("fs", "tp"), to_mate)
    far = lax.optimization_barrier((rest[1].astype(F32) + got[1].astype(F32)).astype(BF16))
    met = rest[0].astype(F32) + got[0].astype(F32)
    met = met + lax.ppermute(far, ("fs", "tp"), to_other).astype(F32)
    takes = lax.rem(z + 1 + q, 2) == 0
    parity = jnp.where(q == lax.rem(z + 1, count), 0, 1)
    mask = takes & (jnp.arange(2) == parity)
    late_part = jnp.where(mask[None, :, None, None], met[:, None], 0.0).reshape(second.shape)
    second = second + other + late_part
    squares = lax.psum(jnp.sum(second * second, axis=(0, 2)), "tp")
    in_vmem = pl.BlockSpec(memory_space=pltpu.VMEM)
    result = pl.pallas_call(
        functools.partial(close_kernel, width=width),
        in_specs=[in_vmem] * 3,
        out_specs=in_vmem,
        out_shape=jax.ShapeDtypeStruct((rows, columns), BF16),
        compiler_params=pltpu.CompilerParams(vmem_limit_bytes=VMEM_LIMIT),
        name="close",
    )(squares.reshape(1, rows), second, own_gain)
    return result.reshape(seq_count, length, columns)


def fits_ring(mesh):
    shape = mesh.shape
    return shape["grp"] == 2 and shape["tp"] == 4 and shape["fs"] == 4


def solution(mesh):
    in_specs = (
        P(("grp", "fs"), None, "tp"),
        P(),
        P("fs", "tp"),
        P("fs", "tp"),
        P("fs", "tp"),
        P(),
        P("tp", "fs"),
        P(),
        P("fs", "tp"),
        P("fs", "tp"),
        P("tp", "fs"),
        P(),
    )
    out_specs = P(("grp", "fs"), None, "tp")
    ring = fits_ring(mesh)
    body = ring_local if ring else plain_local

    return jax.shard_map(body, mesh=mesh, in_specs=in_specs, out_specs=out_specs, check_vma=False)
```

```python
import functools

import jax
import jax.numpy as jnp
from jax import lax
from jax.experimental import pallas as pl
from jax.experimental.pallas import tpu as pltpu
from jax.sharding import PartitionSpec as P


BF16 = jnp.bfloat16
F32 = jnp.float32
VMEM_LIMIT = 20 * 1024 * 1024


def rms_norm(values, gain):
    floats = values.astype(F32)
    scaled = floats * lax.rsqrt(jnp.mean(floats * floats, axis=-1, keepdims=True) + 1e-06)
    return (scaled * gain).astype(BF16)


def plain_local(
    tokens, mix_gain, gate_outer, gate_inner, value_weight, conv_taps, mix_out,
    ffn_gain, ffn_gate, ffn_up, ffn_down, out_gain,
):
    seq_count, length, columns = tokens.shape
    row_count = seq_count * length
    width = columns * lax.axis_size("tp")
    whole = lax.all_gather(tokens, "tp", axis=2, tiled=True).reshape(row_count, width)
    normed = rms_norm(whole, mix_gain)
    channels = gate_outer.shape[1]

    def project(left, weight):
        full = lax.all_gather(weight, "fs", axis=0, tiled=True)
        return jnp.dot(left, full, preferred_element_type=F32)

    outer = project(normed, gate_outer).astype(BF16)
    inner = project(normed, gate_inner).astype(BF16)
    values = project(normed, value_weight).astype(BF16)
    product = (inner.astype(F32) * values.astype(F32)).reshape(seq_count, length, channels)
    own_taps = lax.dynamic_slice_in_dim(conv_taps, lax.axis_index("tp") * channels, channels, 1)
    tap_count = conv_taps.shape[0]
    padded = jnp.pad(product, ((0, 0), (tap_count - 1, 0), (0, 0)))
    conv = jnp.zeros((seq_count, length, channels), F32)
    for offset in range(tap_count):
        conv = conv + own_taps[offset] * padded[:, offset : offset + length]
    gated = (outer.astype(F32) * conv.reshape(row_count, channels)).astype(BF16)
    mix_terms = jnp.dot(
        gated, lax.all_gather(mix_out, "fs", axis=1, tiled=True), preferred_element_type=F32
    )
    mix_full = lax.psum(mix_terms.astype(BF16), "tp").astype(F32)
    first_full = (whole.astype(F32) + mix_full).astype(BF16)
    first = lax.dynamic_slice_in_dim(first_full, lax.axis_index("tp") * columns, columns, 1)
    normed_ffn = rms_norm(first_full, ffn_gain)
    gate = project(normed_ffn, ffn_gate)
    upward = project(normed_ffn, ffn_up)
    hidden = (jax.nn.silu(gate) * upward).astype(BF16)
    down_terms = jnp.dot(
        hidden, lax.all_gather(ffn_down, "fs", axis=1, tiled=True), preferred_element_type=F32
    )
    down_summed = lax.psum_scatter(
        down_terms.astype(BF16), "tp", scatter_dimension=1, tiled=True
    ).astype(F32)
    second = first.astype(F32) + down_summed
    squares = lax.psum(jnp.sum(second * second, axis=1), "tp")
    factor = lax.rsqrt(squares / width + 1e-06)
    own_gain = lax.dynamic_slice_in_dim(out_gain, lax.axis_index("tp") * columns, columns, 0)
    result = second * factor[:, None] * own_gain
    return result.astype(BF16).reshape(seq_count, length, columns)


def dot(left, right):
    return jnp.dot(left, right, preferred_element_type=F32)


def norm_kernel(info, gain, b0, b1, b2, b3, out, *, width):
    q = info[2]
    blocks = [(b, h) for b in (b0, b1, b2, b3) for h in range(2)]
    squares = None
    for b, h in blocks:
        value = b[h].astype(F32)
        squares = value * value if squares is None else squares + value * value
    factor = lax.rsqrt(jnp.sum(squares, axis=-1, keepdims=True) / width + 1e-06)
    for i, (b, h) in enumerate(blocks):
        own = gain[(q ^ (i // 2)) * 2 + h]
        out[i] = (b[h].astype(F32) * factor * own).astype(BF16)


def call(kernel, info, operands, outs, flops):
    in_vmem = pl.BlockSpec(memory_space=pltpu.VMEM)
    moved = 2 * sum(o.size for o in operands)
    return pl.pallas_call(
        kernel,
        in_specs=[pl.BlockSpec(memory_space=pltpu.SMEM)] + [in_vmem] * len(operands),
        out_specs=[in_vmem] * len(outs),
        out_shape=[jax.ShapeDtypeStruct(shape, BF16) for shape in outs],
        cost_estimate=pl.CostEstimate(flops=flops, bytes_accessed=moved, transcendentals=0),
        compiler_params=pltpu.CompilerParams(vmem_limit_bytes=VMEM_LIMIT),
    )(info, *operands)


def norm_call(info, gain, blocks):
    _, rows, half = blocks[0].shape
    width = 8 * half
    kernel = functools.partial(norm_kernel, width=width)
    operands = [gain.reshape(8, 1, half), *blocks]
    return call(kernel, info, operands, [(8, rows, half)], 4000000)[0]


def place(info, step, direction, count):
    z, q = info[0], info[2]
    shard = lax.rem(z + (count - step if direction > 0 else step), count)
    return shard ^ q


def gathered(x, info, pieces, direction, count):
    g = info[1]
    spot = place(info, 0, direction, count)
    parts = [x[2 * spot], x[2 * spot + 1]]
    for step, swapped, _ in pieces:
        spot = place(info, step, direction, count)
        parts.append(x[2 * spot + (1 - g if swapped else g)])
    return jnp.concatenate(parts, axis=1)


def stacked(own, pieces, row, half, columns):
    rows = [own[:, columns]] + [piece[row : row + half, :] for _, _, piece in pieces]
    return jnp.concatenate(rows, axis=0)


def sort_out(keep, give, spot, part, value):
    value = value.astype(BF16)

    @pl.when(lax.rem(spot, 2) == 0)
    def _():
        keep[spot // 2, part] = value

    @pl.when(lax.rem(spot, 2) == 1)
    def _():
        give[spot // 2, part] = value


def mixer_kernel(*refs, count, length):
    info, taps, x, outer_own, inner_own, value_own, mix_own = refs[:7]
    steps = count - 1
    ahead, ahead_y = refs[7 : 7 + steps], refs[7 + steps : 7 + 2 * steps]
    back, back_y = refs[7 + 2 * steps : 7 + 3 * steps], refs[7 + 3 * steps : 7 + 4 * steps]
    keep, give = refs[-2:]
    half = x.shape[2]
    everything = slice(None)
    g = info[1]
    cw = [(k + 1, s, p) for s, group in ((False, ahead), (True, ahead_y)) for k, p in enumerate(group)]
    ccw = [(k + 1, s, p) for s, group in ((False, back), (True, back_y)) for k, p in enumerate(group)]
    left = gathered(x, info, cw, 1, count)
    inner = dot(left, stacked(inner_own, cw, 0, half, everything)).astype(BF16)
    values = dot(left, stacked(value_own, cw, half, half, everything)).astype(BF16)
    left = gathered(x, info, ccw, -1, count)
    outer = dot(left, stacked(outer_own, ccw, 0, half, everything)).astype(BF16)
    product = inner.astype(F32) * values.astype(F32)
    position = lax.broadcasted_iota(jnp.int32, product.shape, 0) % length
    tap_count = taps.shape[0]
    conv = jnp.zeros(product.shape, F32)
    channels = product.shape[1]
    own_taps = taps[:, pl.ds(pl.multiple_of(info[2] * channels, 128), channels)]
    for offset in range(tap_count):
        back_by = tap_count - 1 - offset
        if back_by:
            moved = pltpu.roll(product, back_by, axis=0)
            moved = jnp.where(position >= back_by, moved, 0.0)
        else:
            moved = product
        conv = conv + own_taps[offset][None, :] * moved
    gated = (outer.astype(F32) * conv).astype(BF16)

    own = dot(gated, mix_own[...])
    for h in range(2):
        sort_out(keep, give, place(info, 0, -1, count), h, own[:, h * half : (h + 1) * half])
    for step, swapped, piece in ccw:
        spot = place(info, step, -1, count)
        sort_out(keep, give, spot, 1 - g if swapped else g, dot(gated, piece[half:, :]))


def mixer_call(info, taps, x, owns, cw, cw_y, ccw, ccw_y, count, length):
    _, rows, half = x.shape
    kernel = functools.partial(mixer_kernel, count=count, length=length)
    operands = [taps, x, *owns, *cw, *cw_y, *ccw, *ccw_y]
    flops = 8 * rows * 8 * half * owns[0].shape[1]
    return call(kernel, info, operands, [(2, 2, rows, half)] * 2, flops)


def hidden_kernel(*refs, count, start, size):
    info, x, gate_own, up_own = refs[:4]
    steps = count - 1
    groups = [refs[4 + i * steps : 4 + (i + 1) * steps] for i in range(4)]
    out = refs[-1]
    columns = slice(start, start + size)
    cw = [(k + 1, i == 1, p) for i in (0, 1) for k, p in enumerate(groups[i])]
    ccw = [(k + 1, i == 3, p) for i in (2, 3) for k, p in enumerate(groups[i])]
    half = x.shape[2]
    gate = dot(gathered(x, info, cw, 1, count), stacked(gate_own, cw, 0, half, columns))
    upward = dot(gathered(x, info, ccw, -1, count), stacked(up_own, ccw, 0, half, columns))
    out[...] = (gate / (1.0 + jnp.exp(-gate)) * upward).astype(BF16)


def hidden_call(info, x, gate_own, up_own, cw, cw_y, ccw, ccw_y, count, start, size):
    _, rows, half = x.shape
    kernel = functools.partial(hidden_kernel, count=count, start=start, size=size)
    operands = [x, gate_own, up_own, *cw, *cw_y, *ccw, *ccw_y]
    return call(kernel, info, operands, [(rows, size)], 4 * rows * 8 * half * size)[0]


def split_refs(refs, steps):
    return [refs[i * steps : (i + 1) * steps] for i in range(4)]


def down_product(left, right, weight, split):
    return dot(left[...], weight[:split]) + dot(right[...], weight[split:])


def down_first_kernel(info, left, right, own, cw, cw_y, ccw, ccw_y, keep, give, *, count, split):
    g = info[1]
    rows, piece = keep.shape[-2:]

    def store(step, direction, part, value):
        sort_out(keep, give, place(info, step, direction, count), part, value)

    value = down_product(left, right, own, split)
    for i in range(4):
        store(0, 1, i, value[:, i * piece : (i + 1) * piece])
    weight = jnp.concatenate([p[...] for p in (cw, cw_y, ccw, ccw_y)], axis=1)
    value = down_product(left, right, weight, split)
    for last, direction in enumerate((1, -1)):
        at = 2 * last * piece
        store(1, direction, 2 * g + last, value[:, at : at + piece])
        store(1, direction, 2 * (1 - g) + last, value[:, at + piece : at + 2 * piece])
        for i in range(2):
            store(count - 1, direction, 2 * i + last, jnp.zeros((rows, piece), F32))


def down_next_kernel(*refs, count, split):
    info, left, right, keep_in, give_in = refs[:5]
    steps = count - 3
    groups = split_refs(refs[5 : 5 + 4 * steps], steps)
    keep, give = refs[-2:]
    g = info[1]
    piece = keep.shape[-1]
    keep[...] = keep_in[...]
    give[...] = give_in[...]
    for k in range(steps):
        weight = jnp.concatenate([group[k][...] for group in groups], axis=1)
        value = down_product(left, right, weight, split)
        for last, direction in enumerate((1, -1)):
            at = 2 * last * piece
            spot = place(info, k + 2, direction, count)
            sort_out(keep, give, spot, 2 * g + last, value[:, at : at + piece])
            sort_out(keep, give, spot, 2 * (1 - g) + last, value[:, at + piece : at + 2 * piece])


def down_late_kernel(info, left, right, cw, cw_y, ccw, ccw_y, out, *, count, split):
    g = info[1]
    piece = out.shape[-1]
    weight = jnp.concatenate([p[...] for p in (cw, cw_y, ccw, ccw_y)], axis=1)
    value = down_product(left, right, weight, split).astype(BF16)
    for i, direction in enumerate((1, -1)):
        spot = place(info, count - 1, direction, count) // 2
        out[spot, g] = value[:, 2 * i * piece : (2 * i + 1) * piece]
        out[spot, 1 - g] = value[:, (2 * i + 1) * piece : (2 * i + 2) * piece]


def close_kernel(squares, second, gain, out, *, width):
    rows, piece = second.shape[1:]
    factor = lax.rsqrt(squares[...] / width + 1e-06)
    factor = jnp.broadcast_to(factor, (piece, rows)).T
    for p in range(second.shape[0]):
        out[:, p * piece : (p + 1) * piece] = (second[p] * factor * gain[p]).astype(BF16)


def ring_local(
    tokens, mix_gain, gate_outer, gate_inner, value_weight, conv_taps, mix_out,
    ffn_gain, ffn_gate, ffn_up, ffn_down, out_gain,
):
    count = lax.axis_size("fs")
    seq_count, length, columns = tokens.shape
    rows = seq_count * length
    half = columns // 2
    width = columns * lax.axis_size("tp")
    z, g, q = lax.axis_index("fs"), lax.axis_index("grp"), lax.axis_index("tp")
    info = jnp.stack([z, g, q]).astype(jnp.int32)

    ahead = [(i, (i + 1) % count) for i in range(count)]
    behind = [(d, s) for s, d in ahead]

    def ring(value, pairs):
        arrived, swapped = [], []
        for _ in range(1, count):
            value = lax.ppermute(value, "fs", pairs)
            arrived.append(value)
            swapped.append(lax.ppermute(value, "grp", [(0, 1), (1, 0)]))
        return arrived, swapped

    def mate(value):
        return lax.ppermute(value, "tp", [(i, i ^ 1) for i in range(4)])

    def across(value):
        return lax.ppermute(value, "tp", [(i, i ^ 2) for i in range(4)])

    def gather(own):
        other = across(own)
        return own, mate(own), other, mate(other)

    def rows_of(weight):
        return lax.dynamic_slice_in_dim(weight, g * half, half, 0)

    own_tokens = tokens.reshape(rows, 2, half).transpose(1, 0, 2)
    blocks = gather(own_tokens)

    mix_half = lax.dynamic_slice_in_dim(mix_out, g * half, half, 1)
    m_cw = ring(jnp.concatenate([rows_of(gate_inner), rows_of(value_weight)]), ahead)
    m_ccw = ring(jnp.concatenate([rows_of(gate_outer), mix_half]), behind)
    units = ffn_gate.shape[1]
    split = -(-units // 256) * 128
    gate_half, up_half = rows_of(ffn_gate), rows_of(ffn_up)
    g1 = ring(gate_half[:, :split], ahead)
    u1 = ring(up_half[:, :split], behind)
    g2 = ring(gate_half[:, split:], ahead)
    u2 = ring(up_half[:, split:], behind)
    down_half = lax.dynamic_slice_in_dim(ffn_down, g * half, half, 1)
    d_cw = ring(down_half[:, : half // 2], ahead)
    d_ccw = ring(down_half[:, half // 2 :], behind)

    def scatter(partial):
        keep, got = partial[0], mate(partial[1])
        far = (keep[1].astype(F32) + got[1].astype(F32)).astype(BF16)
        far = lax.optimization_barrier(far)
        near = keep[0].astype(F32) + got[0].astype(F32)
        return near, across(far).astype(F32)

    x = norm_call(info, mix_gain, blocks)
    own_gain = lax.dynamic_slice_in_dim(out_gain, q * columns, columns, 0).reshape(4, 1, half // 2)
    x, own_gain = lax.optimization_barrier((x, own_gain))
    owns = (gate_outer, gate_inner, value_weight, mix_out)
    partial = mixer_call(info, conv_taps, x, owns, *m_cw, *m_ccw, count, length)
    near, other = scatter(partial)
    first = (own_tokens.astype(F32) + (near + other)).astype(BF16)
    blocks = gather(first)
    x = norm_call(info, ffn_gain, blocks)
    left = hidden_call(info, x, ffn_gate, ffn_up, *g1, *u1, count, 0, split)
    right = hidden_call(info, x, ffn_gate, ffn_up, *g2, *u2, count, split, units - split)
    flops = 2 * rows * units * width
    rings = (*d_cw, *d_ccw)
    split_by = {"count": count, "split": split}
    piece = (rows, half // 2)
    kernel = functools.partial(down_first_kernel, **split_by)
    operands = [left, right, ffn_down, *[ring_part[0] for ring_part in rings]]
    partial = call(kernel, info, operands, [(2, 4, *piece)] * 2, flops // 2)
    kernel = functools.partial(down_next_kernel, **split_by)
    operands = [left, right, *partial, *[p for ring_part in rings for p in ring_part[1:-1]]]
    partial = call(kernel, info, operands, [(2, 4, *piece)] * 2, flops // 4)
    second = first.reshape(2, rows, 2, half // 2).transpose(0, 2, 1, 3).reshape(4, rows, half // 2)
    near, other = scatter(partial)
    second = lax.optimization_barrier(second.astype(F32) + near)
    kernel = functools.partial(down_late_kernel, **split_by)
    late = [left, right, *[ring_part[-1] for ring_part in rings]]
    rest = call(kernel, info, late, [(2, 2, *piece)], flops // 4)[0]

    pairs = [(s, i) for s in range(count) for i in range(4)]
    to_mate = [(4 * s + i, 4 * s + (i ^ 1)) for s, i in pairs if (s + 1) % 2 != i % 2]
    to_other = [(4 * s + i, 4 * s + (i ^ 2)) for s, i in pairs if (s + 1) % 2 == i % 2]
    got = lax.ppermute(rest, ("fs", "tp"), to_mate)
    far = lax.optimization_barrier((rest[1].astype(F32) + got[1].astype(F32)).astype(BF16))
    takes = lax.rem(z + 1 + q, 2) == 0
    parity = jnp.where(q == lax.rem(z + 1, count), 0, 1)
    mask = takes & (jnp.arange(2) == parity)

    def late_part(value):
        return jnp.where(mask[None, :, None, None], value[:, None], 0.0).reshape(second.shape)

    crossed = lax.ppermute(far, ("fs", "tp"), to_other)
    second = second + other + late_part(rest[0].astype(F32) + got[0].astype(F32))
    second = lax.optimization_barrier(second)
    second = second + late_part(crossed.astype(F32))
    squares = lax.psum(jnp.sum(second * second, axis=(0, 2)), "tp")
    in_vmem = pl.BlockSpec(memory_space=pltpu.VMEM)
    result = pl.pallas_call(
        functools.partial(close_kernel, width=width),
        in_specs=[in_vmem] * 3,
        out_specs=in_vmem,
        out_shape=jax.ShapeDtypeStruct((rows, columns), BF16),
        compiler_params=pltpu.CompilerParams(vmem_limit_bytes=VMEM_LIMIT),
        name="close",
    )(squares.reshape(1, rows), second, own_gain)
    return result.reshape(seq_count, length, columns)


def fits_ring(mesh):
    shape = mesh.shape
    return shape["grp"] == 2 and shape["tp"] == 4 and shape["fs"] == 4


def solution(mesh):
    in_specs = (
        P(("grp", "fs"), None, "tp"),
        P(),
        P("fs", "tp"),
        P("fs", "tp"),
        P("fs", "tp"),
        P(),
        P("tp", "fs"),
        P(),
        P("fs", "tp"),
        P("fs", "tp"),
        P("tp", "fs"),
        P(),
    )
    out_specs = P(("grp", "fs"), None, "tp")
    ring = fits_ring(mesh)
    body = ring_local if ring else plain_local

    return jax.shard_map(body, mesh=mesh, in_specs=in_specs, out_specs=out_specs, check_vma=False)
```
